32 devices in a mesh: ra: 4 (over y, x), cb: 8 (over z, core).
Axes of the slice: x: 2, y: 2, z: 4, core: 2. Of those that a mesh axis runs over, the one named last changes fastest.
Arguments:
- hidden_states: bfloat16 [384, 4096], P(None, 'ra'), may hold values from -40 to 40
- gain_first: bfloat16 [4096], P('ra'), may hold values from 0.099609375 to 1.8984375
- gate_first: bfloat16 [4096, 11264], P('ra', 'cb'), may hold values from -0.09375 to 0.09375
- up_first: bfloat16 [4096, 11264], P('ra', 'cb'), may hold values from -0.09375 to 0.09375
- down_first: bfloat16 [11264, 4096], P('cb', 'ra'), may hold values from -0.0546875 to 0.0546875
- gain_second: bfloat16 [4096], P('ra'), may hold values from 0.099609375 to 1.8984375
- gate_second: bfloat16 [4096, 11264], P('ra', 'cb'), may hold values from -0.09375 to 0.09375
- up_second: bfloat16 [4096, 11264], P('ra', 'cb'), may hold values from -0.09375 to 0.09375
- down_second: bfloat16 [11264, 4096], P('cb', 'ra'), may hold values from -0.0546875 to 0.0546875
- gain_last: bfloat16 [4096], P('ra'), may hold values from 0.099609375 to 1.8984375
Outputs:
- closed: bfloat16 [384, 4096], P(None, 'ra')
The draws below stay inside these ranges and needn't reach their ends.
All inputs are finite; a program needn't handle non-finite values.
Results may differ from the reference program's by a relative error of at most 0.0098.
Values may be sent and summed in bfloat16 or wider, within the bound.
A program may use at most 64 MiB of HBM per device.

```python
import math
import jax
import jax.numpy as jnp
from jax import lax

D = 4096
FF = 11264
TOKENS = 384


def draw_hidden_states(key, part):
    key_base, key_row, key_col = jax.random.split(key, 3)
    position = jnp.arange(D, dtype=jnp.float32) / D
    rough = jnp.exp(jax.random.uniform(key_col, (D,), jnp.float32, -0.35, 0.35))
    col_scale = 0.5 * jnp.exp(math.log(4.0) * position) * rough
    base = jnp.clip(jax.random.normal(key_base, (TOKENS, D), jnp.float32), -4.0, 4.0)
    row_scale = jnp.exp(jax.random.uniform(key_row, (TOKENS, 1), jnp.float32, math.log(0.3), math.log(3.0)))
    return (base * row_scale * col_scale[None, :]).astype(jnp.bfloat16)


def block_levels(own_key, dims, shards, low, top_value):
    loudness, own = 1.0, jax.random.fold_in(own_key, 6)
    for dim, blocks in shards:
        steps = jnp.exp(jax.random.uniform(jax.random.fold_in(own, dim), (blocks,), jnp.float32, low / len(shards), top_value / len(shards)))
        loudness = loudness * jnp.repeat(steps, dims[dim] // blocks).reshape([-1 if axis == dim else 1 for axis in range(len(dims))])
    return loudness


def centred(own_key, dims, spread, limit, shards=(), kind=jnp.bfloat16):
    result = jax.random.normal(own_key, dims, jnp.float32) * spread
    if len(shards) > 0:
        result = block_levels(own_key, dims, shards, -0.22, 0.18) * result
    return jnp.clip(result, min=-limit, max=limit).astype(kind)


def setup_inputs(seed: int = 0) -> dict:
    keys = jax.random.split(jax.random.key(seed), 11)
    hidden_states = draw_hidden_states(jax.random.fold_in(keys[10], 71), 0)
    gain_first = jnp.clip(1.0 + 0.18 * jax.random.normal(keys[1], (D,), jnp.float32), 0.099609375, 1.8984375).astype(jnp.bfloat16)
    gate_first = centred(keys[2], (D, FF), D ** -0.5, 0.09375, ((0, 4), (1, 8)))
    up_first = centred(keys[3], (D, FF), D ** -0.5, 0.09375, ((0, 4), (1, 8)))
    down_first = centred(keys[4], (FF, D), FF ** -0.5, 0.0546875, ((0, 8), (1, 4)))
    gain_second = jnp.clip(1.0 + 0.18 * jax.random.normal(keys[5], (D,), jnp.float32), 0.099609375, 1.8984375).astype(jnp.bfloat16)
    gate_second = centred(keys[6], (D, FF), D ** -0.5, 0.09375, ((0, 4), (1, 8)))
    up_second = centred(keys[7], (D, FF), D ** -0.5, 0.09375, ((0, 4), (1, 8)))
    down_second = centred(keys[8], (FF, D), FF ** -0.5, 0.0546875, ((0, 8), (1, 4)))
    gain_last = jnp.clip(1.0 + 0.18 * jax.random.normal(keys[9], (D,), jnp.float32), 0.099609375, 1.8984375).astype(jnp.bfloat16)
    return {"hidden_states": hidden_states, "gain_first": gain_first, "gate_first": gate_first, "up_first": up_first, "down_first": down_first, "gain_second": gain_second, "gate_second": gate_second, "up_second": up_second, "down_second": down_second, "gain_last": gain_last}


norm_eps = 1e-06
residual_weight = 0.25
branch_weight = 0.5

def half_step(stream, gain, w_gate, w_up, w_down):
    values = stream.astype(jnp.float32)
    scale = lax.rsqrt(lax.optimization_barrier(jnp.mean(values * values, axis=1, keepdims=True)) + norm_eps)
    normed = (values * gain.astype(jnp.float32)).astype(jnp.bfloat16)
    gate = jnp.dot(normed, w_gate, preferred_element_type=jnp.float32) * scale
    upper = jnp.dot(normed, w_up, preferred_element_type=jnp.float32) * scale
    hidden = (jax.nn.silu(gate) * upper).astype(jnp.bfloat16)
    branch = jnp.dot(hidden, w_down, preferred_element_type=jnp.float32)
    return (residual_weight * values + branch_weight * branch).astype(jnp.bfloat16)

def reference(hidden_states, gain_first, gate_first, up_first, down_first, gain_second, gate_second, up_second, down_second, gain_last):
    first = half_step(hidden_states, gain_first, gate_first, up_first, down_first)
    second = half_step(first, gain_second, gate_second, up_second, down_second)
    values = second.astype(jnp.float32)
    scale = lax.rsqrt(lax.optimization_barrier(jnp.mean(values * values, axis=1, keepdims=True)) + norm_eps)
    return (values * scale * gain_last.astype(jnp.float32)).astype(jnp.bfloat16)
```

```python
import functools

import jax
import jax.numpy as jnp
from jax import lax
from jax.experimental import pallas as pl
from jax.experimental.pallas import tpu as pltpu
from jax.sharding import PartitionSpec as P

norm_eps = 1e-06
residual_weight = 0.25
branch_weight = 0.5


def half_step(stream, gain, w_gate, w_up, w_down):
    width = stream.shape[1] * lax.axis_size("ra")
    values = stream.astype(jnp.float32)
    local_squares = jnp.sum(values * values, axis=1)
    normed = (values * gain.astype(jnp.float32)).astype(jnp.bfloat16)
    gate_part = jnp.dot(normed, w_gate, preferred_element_type=jnp.float32)
    upper_part = jnp.dot(normed, w_up, preferred_element_type=jnp.float32)
    count_ra = lax.axis_size("ra")
    spread_squares = jnp.broadcast_to(local_squares[:, None], (stream.shape[0], count_ra))
    gate, upper, squares = (
        lax.psum_scatter(gate_part, "ra", scatter_dimension=1, tiled=True),
        lax.psum_scatter(upper_part, "ra", scatter_dimension=1, tiled=True),
        lax.psum_scatter(spread_squares, "ra", scatter_dimension=1, tiled=True),
    )
    scale = lax.rsqrt(squares / width + norm_eps)
    hidden = (jax.nn.silu(gate * scale) * (upper * scale)).astype(jnp.bfloat16)
    branch = jnp.dot(
        lax.all_gather(hidden, "ra", axis=1, tiled=True), w_down, preferred_element_type=jnp.float32
    )
    block = lax.psum_scatter(branch, "cb", scatter_dimension=0, tiled=True)
    count = block.shape[0]
    offset = lax.axis_index("cb") * count
    own_rows = lax.dynamic_slice_in_dim(values, offset, count, 0)
    updated = (residual_weight * own_rows + branch_weight * block).astype(jnp.bfloat16)
    return lax.all_gather(updated, "cb", axis=0, tiled=True)


def body(
    hidden_states,
    gain_first,
    gate_first,
    up_first,
    down_first,
    gain_second,
    gate_second,
    up_second,
    down_second,
    gain_last,
):
    first = half_step(hidden_states, gain_first, gate_first, up_first, down_first)
    second = half_step(first, gain_second, gate_second, up_second, down_second)
    width = second.shape[1] * lax.axis_size("ra")
    values = second.astype(jnp.float32)
    squares = lax.psum(jnp.sum(values * values, axis=1), "ra")
    scale = lax.rsqrt(squares / width + norm_eps)[:, None]
    return (values * scale * gain_last.astype(jnp.float32)).astype(jnp.bfloat16)


MESH = pl.DeviceIdType.MESH
CORES = 2
LANES = 128
SUBLANES = 8
STEP = 64
LETTERS = "ASBCRDEFGHYZ"
ROLES = ("gate", "up", "sum", "squares", "left", "right", "hidden", "pair", "mix", "spread", "rows")
GROUP = {"gate": 0, "up": 0, "sum": 0, "squares": 1, "left": 2, "right": 2, "hidden": 2, "pair": 3, "mix": 4, "spread": 5, "rows": 6}
LONG, HOP = ("gate", "up"), ("left", "right")
SEQUENCE = (0, 1, 24, 25, 2, 48, 26, 49, 3, 4, 50, 27, 28, 72, 5, 73, 51, 29, 52, 74, 6, 96, 53, 7, 30, 97, 120, 75, 31, 98, 54, 76, 121, 55, 8, 122, 77, 99, 100, 32, 123, 124, 78, 56, 101, 79, 9, 125, 12, 33, 102, 13, 36, 57, 103, 126, 37, 14, 80, 127, 60, 38, 61, 15, 104, 16, 62, 81, 39, 40, 128, 84, 17, 85, 63, 105, 41, 64, 86, 18, 129, 108, 65, 19, 42, 109, 132, 87, 43, 110, 66, 88, 133, 67, 20, 134, 89, 111, 112, 44, 135, 136, 90, 68, 113, 91, 21, 137, 22, 45, 114, 46, 115, 138, 69, 23, 139, 70, 92, 47, 116, 71, 140, 93, 94, 117, 118, 141, 95, 142, 119, 143)


def plan(mesh, tokens, width, units):
    n, devices = mesh.shape["ra"], mesh.shape["cb"]
    if n != 4 or devices % CORES or devices < 2 * CORES or tokens % STEP or STEP % (devices * SUBLANES) or STEP % (n * 2 * SUBLANES):
        return None
    if width % (n * LANES) or units % (devices * LANES):
        return None
    return STEP


def ring_index(position):
    return position ^ (position >> 1)


def order(chunks):
    stages = [(c, b, s) for c in range(chunks) for b in range(2) for s in range(len(LETTERS)) if b or LETTERS[s] not in "YZ"]
    if len(SEQUENCE) == len(stages):
        return [(x // 24, x // 12 % 2, LETTERS[x % 12]) for x in SEQUENCE]
    return [(c, b, LETTERS[s]) for b, s, c in sorted((b, s, c) for c, b, s in stages)]


def kernel(n, nz, chunks, tc, width, x_hbm, g1_ref, wg1, wu1, wd1, g2_ref, wg2, wu2, wd2, g3_ref, out_ref,
           wg_a, wu_a, wd_a, wg_b, wu_b, wd_b, x_ref, mid, end, act, part, long_in, short_in, hid, sq_own, sq_in,
           down, pair_in, mixed, z_in, x_sem, w_sem, send_sem, recv_sem):
    f32, bf16 = jnp.float32, jnp.bfloat16
    ra, cb = lax.axis_index("ra"), lax.axis_index("cb")
    pos, z, core = ring_index(ra), cb // CORES, cb % CORES
    local, units = x_ref.shape[-1], hid.shape[-1]
    r, half_rows, q = tc // n, tc // CORES, tc // (CORES * nz)
    streams = (x_ref, mid, end)
    gains = (g1_ref, g2_ref, g3_ref)
    weights = ((wg_a, wu_a, wd_a), (wg_b, wu_b, wd_b))

    loads = [[pltpu.make_async_copy(src, dst, w_sem.at[b, i]) for i, (src, dst) in enumerate(zip(srcs, weights[b]))]
             for b, srcs in enumerate(((wg1, wu1, wd1), (wg2, wu2, wd2)))]
    first, others_x = pl.ds(0, tc), pl.ds(tc, (chunks - 1) * tc)
    x_loads = [pltpu.make_async_copy(x_hbm.at[part_x], x_ref.at[part_x], x_sem.at[i]) for i, part_x in enumerate((first, others_x))]
    x_loads[0].start()
    for load in loads[0][:2]:
        load.start()
    x_loads[1].start()
    pending = {(b, i): loads[b][i] for b in range(2) for i in range(3)}

    def ready(b, i):
        if (b, i) in pending:
            pending.pop((b, i)).wait()

    def at(position):
        return lax.rem(position + 2 * n, n)

    def ring(position):
        return (ring_index(at(position)), cb)

    steps = (ring(pos + 1), ring(pos - 1))
    signs = (1, -1)
    partner = (ra, z * CORES + (1 - core))
    others = [ring(pos + d) for d in range(1, n)]
    planes = [lax.rem(z + d, nz) for d in range(1, nz)]
    layers = [(ra, plane * CORES + core) for plane in planes]

    barrier = pltpu.get_barrier_semaphore()
    peers = others + layers + [partner]
    for peer in peers:
        pl.semaphore_signal(barrier, inc=1, device_id=peer, device_id_type=MESH)

    def send(role, c, src, dst, device):
        pltpu.make_async_remote_copy(src_ref=src, dst_ref=dst, send_sem=send_sem.at[GROUP[role]], recv_sem=recv_sem.at[c, ROLES.index(role)],
                                     device_id=device, device_id_type=MESH).start()

    def take(role, c, view):
        copy = pltpu.make_async_remote_copy(src_ref=view, dst_ref=view, send_sem=send_sem.at[0], recv_sem=recv_sem.at[c, ROLES.index(role)],
                                            device_id=partner, device_id_type=MESH)
        copy.wait_recv()

    def sent(group, view):
        copy = pltpu.make_async_remote_copy(src_ref=view, dst_ref=view, send_sem=send_sem.at[group], recv_sem=recv_sem.at[0, 0],
                                            device_id=partner, device_id_type=MESH)
        copy.wait_send()

    def rows(c, offset, count):
        return pl.ds(pl.multiple_of(c * tc + offset, SUBLANES), count)

    def stage_a(b, c):
        whole = pl.ds(c * tc, tc)
        if b:
            take("rows", c, pair_in.at[0, pl.ds(0, half_rows)])
        values = streams[b][whole, :].astype(f32)
        act[b, whole, :] = (values * gains[b][...].astype(f32)).astype(bf16)
        far = at(pos + 2)
        for half in range(2):
            ready(b, half)
            part[b, half, whole, :] = jnp.dot(act[b, whole, :], weights[b][half][...], preferred_element_type=f32).astype(bf16)
            if not b and not c and not half:
                pl.semaphore_wait(barrier, len(peers))
            send(LONG[half], c, part.at[b, half, rows(c, far * r, r)], long_in.at[b, half, 0, pl.ds(c * r, r)], steps[half])
        if not b and not c:
            for load in loads[0][2:] + loads[1]:
                load.start()
            x_loads[1].wait()

    def send_squares(b, c, values):
        squares = values * values
        folded = squares[:, :LANES]
        for k in range(1, local // LANES):
            folded = folded + squares[:, k * LANES:(k + 1) * LANES]
        sq_own[b, c, :, :tc] = jnp.sum(folded.T, axis=0, keepdims=True)
        for d in range(n - 1):
            send("squares", c, sq_own.at[b, c], sq_in.at[b, c, d], others[d])

    def scales(b, c):
        total = sq_own[b, c, :, :tc]
        take("squares", c, sq_in.at[b, c])
        for d in range(n - 1):
            total = total + sq_in[b, c, d, :, :tc]
        scale = lax.rsqrt(total / width + norm_eps)
        return jnp.broadcast_to(scale, (LANES, tc)).T

    def stage_s(b, c):
        for side in range(2):
            half = 1 - side
            send("sum", c, part.at[b, half, rows(c, at(pos + signs[side]) * r, r)], short_in.at[b, half, pl.ds(c * r, r)], steps[side])
        send_squares(b, c, streams[b][pl.ds(c * tc, tc), :].astype(f32))

    def stage_b(b, c):
        for half in range(2):
            take(LONG[half], c, short_in.at[0, 0, pl.ds(0, r)])
            owner = rows(c, at(pos + signs[half]) * r, r)
            box = pl.ds(c * r, r)
            part[b, half, owner, :] = (part[b, half, owner, :].astype(f32) + long_in[b, half, 0, box, :].astype(f32)).astype(bf16)
            send("sum", c, part.at[b, half, owner], long_in.at[b, half, 1, box], steps[half])

    def stage_c(b, c):
        spread = scales(b, c).reshape(n, r, LANES)
        scale = spread[0]
        for k in range(1, n):
            scale = jnp.where(pos == k, spread[k], scale)
        scale = scale[:, :1]
        own, box = rows(c, pos * r, r), pl.ds(c * r, r)
        take("sum", c, hid.at[0, pl.ds(0, n * r)])
        sums = []
        for half in range(2):
            sums.append((part[b, half, own, :].astype(f32) + short_in[b, half, box, :].astype(f32)
                         + long_in[b, half, 1, box, :].astype(f32)) * scale)
        hid[b, own, :] = (jax.nn.silu(sums[0]) * sums[1]).astype(bf16)
        views = [hid.at[b, rows(c, pos * r + half * (r // 2), r // 2)] for half in range(2)]
        for side in range(2):
            send(HOP[side], c, views[side], views[side], steps[side])

    def stage_r(b, c):
        views = [hid.at[b, rows(c, pos * r + half * (r // 2), r // 2)] for half in range(2)]
        for side in range(2):
            send("hidden", c, views[1 - side], views[1 - side], steps[side])

    def stage_d(b, c):
        for side in range(2):
            take(HOP[side], c, hid.at[0, pl.ds(0, r // 2)])
            view = hid.at[b, rows(c, at(pos - signs[side]) * r + side * (r // 2), r // 2)]
            send("hidden", c, view, view, steps[side])

    def stage_e(b, c):
        whole = pl.ds(c * tc, tc)
        ready(b, 2)
        take("hidden", c, hid.at[0, pl.ds(0, 2 * r)])
        down[b, whole, :] = jnp.dot(hid[b, whole, :], weights[b][2][...], preferred_element_type=f32).astype(bf16)
        send("pair", c, down.at[b, rows(c, (1 - core) * half_rows, half_rows)],
             pair_in.at[b, pl.ds(c * half_rows, half_rows)], partner)

    def stage_f(b, c):
        take("pair", c, pair_in.at[0, pl.ds(0, half_rows)])
        box = pl.ds(c * half_rows, half_rows)
        both = down[b, rows(c, core * half_rows, half_rows), :].astype(f32) + pair_in[b, box, :].astype(f32)
        mixed[b, box, :] = both.astype(bf16)
        for d in range(nz - 1):
            send("mix", c, mixed.at[b, pl.ds(pl.multiple_of(c * half_rows + planes[d] * q, SUBLANES), q)], z_in.at[b, d, pl.ds(c * q, q)], layers[d])

    def stage_g(b, c):
        total = mixed[b, pl.ds(pl.multiple_of(c * half_rows + z * q, SUBLANES), q), :].astype(f32)
        take("mix", c, pair_in.at[0, pl.ds(0, (nz - 1) * q)])
        for d in range(nz - 1):
            total = total + z_in[b, d, pl.ds(c * q, q), :].astype(f32)
        own = rows(c, core * half_rows + z * q, q)
        after = streams[b + 1]
        after[own, :] = (residual_weight * streams[b][own, :].astype(f32) + branch_weight * total).astype(bf16)
        view = after.at[own]
        for d in range(nz - 1):
            send("spread", c, view, view, layers[d])

    def stage_h(b, c):
        take("spread", c, pair_in.at[0, pl.ds(0, (nz - 1) * q)])
        view = streams[b + 1].at[rows(c, core * half_rows, half_rows)]
        send("rows", c, view, view, partner)

    def stage_y(b, c):
        take("rows", c, pair_in.at[0, pl.ds(0, half_rows)])
        send_squares(b + 1, c, end[pl.ds(c * tc, tc), :].astype(f32))

    def stage_z(b, c):
        whole = pl.ds(c * tc, tc)
        scale = scales(b + 1, c)[:, :1]
        out_ref[whole, :] = (end[whole, :].astype(f32) * scale * gains[2][...].astype(f32)).astype(bf16)

    stages = dict(zip(LETTERS, (stage_a, stage_s, stage_b, stage_c, stage_r, stage_d, stage_e, stage_f, stage_g, stage_h,
                                stage_y, stage_z)))
    x_loads[0].wait()
    for c, b, s in order(chunks):
        stages[s](b, c)
    most = pl.ds(0, 3 * r * chunks)
    for group, view in enumerate((part.at[:, :, most], sq_in, part.at[:, 0, most], pair_in, z_in, z_in, pair_in)):
        sent(group, view)


def fused_body(n, devices, tc, width, hidden_states, gain_first, gate_first, up_first, down_first, gain_second, gate_second,
               up_second, down_second, gain_last):
    tokens, local = hidden_states.shape
    units = gate_first.shape[1]
    chunks, nz = tokens // tc, devices // CORES
    bf16 = jnp.bfloat16
    share = tokens // n
    vmem = pl.BlockSpec(memory_space=pltpu.VMEM)
    hbm = pl.BlockSpec(memory_space=pl.ANY)
    return pl.pallas_call(
        functools.partial(kernel, n, nz, chunks, tc, width),
        out_shape=pltpu.VMEM((tokens, local), bf16),
        in_specs=[hbm, vmem, hbm, hbm, hbm, vmem, hbm, hbm, hbm, vmem],
        out_specs=vmem,
        scratch_shapes=[pltpu.VMEM(w.shape, bf16) for w in (gate_first, up_first, down_first, gate_second, up_second, down_second)]
        + [
            pltpu.VMEM((tokens, local), bf16),
            pltpu.VMEM((tokens, local), bf16),
            pltpu.VMEM((tokens, local), bf16),
            pltpu.VMEM((2, tokens, local), bf16),
            pltpu.VMEM((2, 2, tokens, units), bf16),
            pltpu.VMEM((2, 2, 2, share, units), bf16),
            pltpu.VMEM((2, 2, share, units), bf16),
            pltpu.VMEM((2, tokens, units), bf16),
            pltpu.VMEM((3, chunks, 1, LANES), jnp.float32),
            pltpu.VMEM((3, chunks, n - 1, 1, LANES), jnp.float32),
            pltpu.VMEM((2, tokens, local), bf16),
            pltpu.VMEM((2, tokens // CORES, local), bf16),
            pltpu.VMEM((2, tokens // CORES, local), bf16),
            pltpu.VMEM((2, nz - 1, tokens // devices, local), bf16),
            pltpu.SemaphoreType.DMA((2,)),
            pltpu.SemaphoreType.DMA((2, 3)),
            pltpu.SemaphoreType.DMA((max(GROUP.values()) + 1,)),
            pltpu.SemaphoreType.DMA((chunks, len(ROLES))),
        ],
        compiler_params=pltpu.CompilerParams(collective_id=0, has_side_effects=True),
    )(
        hidden_states, gain_first, gate_first, up_first, down_first,
        gain_second, gate_second, up_second, down_second, gain_last,
    )


def solution(mesh):
    in_specs = (
        P(None, "ra"),
        P("ra"),
        P("ra", "cb"),
        P("ra", "cb"),
        P("cb", "ra"),
        P("ra"),
        P("ra", "cb"),
        P("ra", "cb"),
        P("cb", "ra"),
        P("ra"),
    )

    def run(hidden_states, *rest):
        tokens, width = hidden_states.shape
        tc = plan(mesh, tokens, width, rest[1].shape[1])
        form = body
        if tc is not None:
            form = functools.partial(fused_body, mesh.shape["ra"], mesh.shape["cb"], tc, width)
        return jax.shard_map(form, mesh=mesh, in_specs=in_specs, out_specs=P(None, "ra"), check_vma=False)(hidden_states, *rest)

    return run
```

```python
import functools

import jax
import jax.numpy as jnp
from jax import lax
from jax.experimental import pallas as pl
from jax.experimental.pallas import tpu as pltpu
from jax.sharding import PartitionSpec as P

norm_eps = 1e-06
residual_weight = 0.25
branch_weight = 0.5


def half_step(stream, gain, w_gate, w_up, w_down):
    width = stream.shape[1] * lax.axis_size("ra")
    values = stream.astype(jnp.float32)
    local_squares = jnp.sum(values * values, axis=1)
    normed = (values * gain.astype(jnp.float32)).astype(jnp.bfloat16)
    gate_part = jnp.dot(normed, w_gate, preferred_element_type=jnp.float32)
    upper_part = jnp.dot(normed, w_up, preferred_element_type=jnp.float32)
    count_ra = lax.axis_size("ra")
    spread_squares = jnp.broadcast_to(local_squares[:, None], (stream.shape[0], count_ra))
    gate, upper, squares = (
        lax.psum_scatter(gate_part, "ra", scatter_dimension=1, tiled=True),
        lax.psum_scatter(upper_part, "ra", scatter_dimension=1, tiled=True),
        lax.psum_scatter(spread_squares, "ra", scatter_dimension=1, tiled=True),
    )
    scale = lax.rsqrt(squares / width + norm_eps)
    hidden = (jax.nn.silu(gate * scale) * (upper * scale)).astype(jnp.bfloat16)
    branch = jnp.dot(
        lax.all_gather(hidden, "ra", axis=1, tiled=True), w_down, preferred_element_type=jnp.float32
    )
    block = lax.psum_scatter(branch, "cb", scatter_dimension=0, tiled=True)
    count = block.shape[0]
    offset = lax.axis_index("cb") * count
    own_rows = lax.dynamic_slice_in_dim(values, offset, count, 0)
    updated = (residual_weight * own_rows + branch_weight * block).astype(jnp.bfloat16)
    return lax.all_gather(updated, "cb", axis=0, tiled=True)


def body(
    hidden_states,
    gain_first,
    gate_first,
    up_first,
    down_first,
    gain_second,
    gate_second,
    up_second,
    down_second,
    gain_last,
):
    first = half_step(hidden_states, gain_first, gate_first, up_first, down_first)
    second = half_step(first, gain_second, gate_second, up_second, down_second)
    width = second.shape[1] * lax.axis_size("ra")
    values = second.astype(jnp.float32)
    squares = lax.psum(jnp.sum(values * values, axis=1), "ra")
    scale = lax.rsqrt(squares / width + norm_eps)[:, None]
    return (values * scale * gain_last.astype(jnp.float32)).astype(jnp.bfloat16)


MESH = pl.DeviceIdType.MESH
CORES = 2
LANES = 128
SUBLANES = 8
PLANES = 4
OWNERS = 2
STEP = 64
LETTERS = "AUSBVCRDWEFGHZ"
ROLES = ("gate", "up", "sum", "squares", "left", "right", "hidden", "pair", "mix", "spread", "rows", "closing")
GROUP = {"gate": 0, "up": 0, "sum": 0, "squares": 1, "left": 2, "right": 2, "hidden": 2, "pair": 3, "rows": 3, "mix": 4, "spread": 5, "closing": 6}
LONG, HOP = ("gate", "up"), ("left", "right")
SEQUENCE = (0, 1, 2, 28, 29, 30, 3, 56, 4, 57, 84, 31, 58, 32, 5, 6, 59, 112, 60, 85, 33, 8, 7, 34, 113, 140, 61, 88, 35, 36, 86, 9, 62, 141, 87, 64, 63, 115, 10, 114, 116, 37, 89, 142, 38, 65, 143, 144, 90, 11, 117, 91, 92, 66, 39, 118, 145, 119, 12, 120, 146, 93, 67, 14, 148, 147, 15, 40, 94, 16, 121, 42, 43, 44, 68, 122, 149, 18, 17, 70, 95, 71, 46, 150, 123, 45, 72, 19, 20, 96, 73, 74, 47, 151, 124, 48, 98, 99, 22, 100, 21, 126, 50, 127, 75, 49, 152, 101, 102, 76, 154, 128, 155, 78, 77, 51, 156, 23, 52, 129, 130, 24, 103, 157, 158, 104, 79, 80, 53, 131, 106, 105, 25, 132, 159, 160, 134, 133, 161, 162, 81, 54, 107, 108, 135, 136, 163, 164, 55, 26, 109, 137, 165, 110, 82, 27, 138, 166, 139, 111, 83, 167)


def plan(mesh, tokens, width, units):
    n, devices = mesh.shape["ra"], mesh.shape["cb"]
    if n != 4 or devices != PLANES * CORES or tokens % STEP or STEP > LANES or STEP % (OWNERS * SUBLANES) or STEP % (n * 2 * SUBLANES):
        return None
    if width % (n * LANES) or units % (devices * LANES):
        return None
    return STEP


def ring_index(position):
    return position ^ (position >> 1)


def order(chunks):
    stages = [(c, b, s) for c in range(chunks) for b in range(2) for s in range(len(LETTERS)) if b or LETTERS[s] != "Z"]
    if len(SEQUENCE) == len(stages):
        return [(x // 28, x // 14 % 2, LETTERS[x % 14]) for x in SEQUENCE]
    return [(c, b, LETTERS[s]) for b, s, c in sorted((b, s, c) for c, b, s in stages)]


def kernel(n, chunks, tc, width, x_hbm, g1_ref, wg1, wu1, wd1, g2_ref, wg2, wu2, wd2, g3_ref, out_ref,
           wg_a, wu_a, wd_a, wg_b, wu_b, wd_b, x_ref, mid, end, act, part, long_in, short_in, hid, sq_own, sq_in, sq_end,
           down, pair_in, mixed, z_in, x_sem, w_sem, send_sem, recv_sem):
    f32, bf16 = jnp.float32, jnp.bfloat16
    ra, cb = lax.axis_index("ra"), lax.axis_index("cb")
    pos, z, core = ring_index(ra), cb // CORES, cb % CORES
    local, units = x_ref.shape[-1], hid.shape[-1]
    r, q = tc // n, tc // OWNERS
    middle = (z == 1) | (z == 2)
    adds = core == 1
    owns = adds & middle
    streams = (x_ref, mid, end)
    gains = (g1_ref, g2_ref, g3_ref)
    weights = ((wg_a, wu_a, wd_a), (wg_b, wu_b, wd_b))

    loads = [[pltpu.make_async_copy(src, dst, w_sem.at[b, i]) for i, (src, dst) in enumerate(zip(srcs, weights[b]))]
             for b, srcs in enumerate(((wg1, wu1, wd1), (wg2, wu2, wd2)))]
    first, others_x = pl.ds(0, 2 * tc), pl.ds(2 * tc, (chunks - 2) * tc)
    x_loads = [pltpu.make_async_copy(x_hbm.at[part_x], x_ref.at[part_x], x_sem.at[i]) for i, part_x in enumerate((first, others_x))]
    x_loads[0].start()
    for load in loads[0][:2]:
        load.start()
    x_loads[1].start()
    pending = {(b, i): loads[b][i] for b in range(2) for i in range(3)}

    def ready(b, i):
        if (b, i) in pending:
            pending.pop((b, i)).wait()

    def at(position):
        return lax.rem(position + 2 * n, n)

    def ring(position):
        return (ring_index(at(position)), cb)

    steps = (ring(pos + 1), ring(pos - 1))
    signs = (1, -1)
    partner = (ra, z * CORES + (1 - core))
    others = [ring(pos + d) for d in range(1, n)]
    layers = [(ra, lax.rem(z + d, PLANES) * CORES + core) for d in range(1, PLANES)]

    def layer(plane):
        return (ra, plane * CORES + core)

    barrier = pltpu.get_barrier_semaphore()
    peers = others + layers + [partner]
    for peer in peers:
        pl.semaphore_signal(barrier, inc=1, device_id=peer, device_id_type=MESH)

    def send(role, c, src, dst, device):
        pltpu.make_async_remote_copy(src_ref=src, dst_ref=dst, send_sem=send_sem.at[GROUP[role]], recv_sem=recv_sem.at[c, ROLES.index(role)],
                                     device_id=device, device_id_type=MESH).start()

    def take(role, c, view):
        copy = pltpu.make_async_remote_copy(src_ref=view, dst_ref=view, send_sem=send_sem.at[0], recv_sem=recv_sem.at[c, ROLES.index(role)],
                                            device_id=partner, device_id_type=MESH)
        copy.wait_recv()

    def sent(group, view):
        copy = pltpu.make_async_remote_copy(src_ref=view, dst_ref=view, send_sem=send_sem.at[group], recv_sem=recv_sem.at[0, 0],
                                            device_id=partner, device_id_type=MESH)
        copy.wait_send()

    greeted = []

    def rows(c, offset, count):
        return pl.ds(pl.multiple_of(c * tc + offset, SUBLANES), count)

    def receive_rows(c):
        @pl.when(jnp.logical_not(adds))
        def _():
            take("rows", c, act.at[0, pl.ds(0, tc)])

    def stage_a(b, c):
        whole = pl.ds(c * tc, tc)
        if b:
            receive_rows(c)
        elif c > 1 and len(x_loads) > 1:
            x_loads.pop().wait()
        values = streams[b][whole, :].astype(f32)
        act[b, whole, :] = (values * gains[b][...].astype(f32)).astype(bf16)
        project(b, c, 0)

    def stage_u(b, c):
        project(b, c, 1)

    def project(b, c, half):
        whole = pl.ds(c * tc, tc)
        ready(b, half)
        part[b, half, whole, :] = jnp.dot(act[b, whole, :], weights[b][half][...], preferred_element_type=f32).astype(bf16)
        if not greeted:
            greeted.append(True)
            pl.semaphore_wait(barrier, len(peers))
        send(LONG[half], c, part.at[b, half, rows(c, at(pos + 2) * r, r)], long_in.at[b, half, 0, pl.ds(c * r, r)], steps[half])
        if half and len(greeted) == 1:
            greeted.append(True)
            for load in loads[0][2:] + loads[1]:
                load.start()

    def fold(values):
        squares = values * values
        folded = squares[:, :LANES]
        for k in range(1, local // LANES):
            folded = folded + squares[:, k * LANES:(k + 1) * LANES]
        return folded

    def column(squares):
        return jnp.broadcast_to(lax.rsqrt(squares / width + norm_eps), (LANES, tc)).T

    def send_squares(b, c, values):
        sq_own[b, c, :, :tc] = jnp.sum(fold(values).T, axis=0, keepdims=True)
        for d in range(n - 1):
            send("squares", c, sq_own.at[b, c], sq_in.at[b, c, d], others[d])

    def scales(b, c):
        total = sq_own[b, c, :, :tc]
        take("squares", c, sq_in.at[b, c])
        for d in range(n - 1):
            total = total + sq_in[b, c, d, :, :tc]
        return column(total)

    def stage_s(b, c):
        for side in range(2):
            half = 1 - side
            send("sum", c, part.at[b, half, rows(c, at(pos + signs[side]) * r, r)], short_in.at[b, half, pl.ds(c * r, r)], steps[side])
        send_squares(b, c, streams[b][pl.ds(c * tc, tc), :].astype(f32))

    def pass_on(b, c, half):
        take(LONG[half], c, short_in.at[0, 0, pl.ds(0, r)])
        owner = rows(c, at(pos + signs[half]) * r, r)
        box = pl.ds(c * r, r)
        part[b, half, owner, :] = (part[b, half, owner, :].astype(f32) + long_in[b, half, 0, box, :].astype(f32)).astype(bf16)
        send("sum", c, part.at[b, half, owner], long_in.at[b, half, 1, box], steps[half])

    def stage_b(b, c):
        pass_on(b, c, 0)

    def stage_v(b, c):
        pass_on(b, c, 1)

    def stage_c(b, c):
        spread = scales(b, c).reshape(n, r, LANES)
        scale = spread[0]
        for k in range(1, n):
            scale = jnp.where(pos == k, spread[k], scale)
        scale = scale[:, :1]
        own, box = rows(c, pos * r, r), pl.ds(c * r, r)
        take("sum", c, hid.at[0, pl.ds(0, n * r)])
        sums = []
        for half in range(2):
            sums.append((part[b, half, own, :].astype(f32) + short_in[b, half, box, :].astype(f32)
                         + long_in[b, half, 1, box, :].astype(f32)) * scale)
        hid[b, own, :] = (jax.nn.silu(sums[0]) * sums[1]).astype(bf16)
        views = [hid.at[b, rows(c, pos * r + half * (r // 2), r // 2)] for half in range(2)]
        for side in range(2):
            send(HOP[side], c, views[side], views[side], steps[side])

    def stage_r(b, c):
        views = [hid.at[b, rows(c, pos * r + half * (r // 2), r // 2)] for half in range(2)]
        for side in range(2):
            send("hidden", c, views[1 - side], views[1 - side], steps[side])

    def hop(b, c, side):
        take(HOP[side], c, hid.at[0, pl.ds(0, r // 2)])
        view = hid.at[b, rows(c, at(pos - signs[side]) * r + side * (r // 2), r // 2)]
        send("hidden", c, view, view, steps[side])

    def stage_d(b, c):
        hop(b, c, 0)

    def stage_w(b, c):
        hop(b, c, 1)

    def stage_e(b, c):
        whole = pl.ds(c * tc, tc)
        ready(b, 2)
        take("hidden", c, hid.at[0, pl.ds(0, 2 * r)])
        down[b, whole, :] = jnp.dot(hid[b, whole, :], weights[b][2][...], preferred_element_type=f32).astype(bf16)

        @pl.when(jnp.logical_not(adds))
        def _():
            send("pair", c, down.at[b, whole], pair_in.at[b, whole], partner)

    def stage_f(b, c):
        whole = pl.ds(c * tc, tc)

        def mix(plane):
            send("mix", c, mixed.at[b, rows(c, (plane - 1) * q, q)],
                 z_in.at[b, lax.rem(z - plane + PLANES, PLANES) - 1, pl.ds(c * q, q)], layer(plane))

        first_owner = jnp.where(z < 2, 2, 1)

        @pl.when(adds)
        def _():
            take("pair", c, act.at[0, whole])
            mixed[b, whole, :] = (down[b, whole, :].astype(f32) + pair_in[b, whole, :].astype(f32)).astype(bf16)
            mix(first_owner)

        @pl.when(adds & jnp.logical_not(middle))
        def _():
            mix(PLANES - 1 - first_owner)

    def stage_g(b, c):
        @pl.when(owns)
        def _():
            part_of = z - 1
            own = rows(c, part_of * q, q)
            total = mixed[b, own, :].astype(f32)
            take("mix", c, act.at[0, pl.ds(0, (PLANES - 1) * q)])
            for d in range(PLANES - 1):
                total = total + z_in[b, d, pl.ds(c * q, q), :].astype(f32)
            after = streams[b + 1]
            rounded = (residual_weight * streams[b][own, :].astype(f32) + branch_weight * total).astype(bf16)
            after[own, :] = rounded
            view = after.at[own]
            near = jnp.where(z == 1, 0, PLANES - 1)
            for plane in (PLANES - 1 - near, near, PLANES - 1 - z):
                send("spread", c, view, view, layer(plane))
            if b:
                folded = fold(rounded.astype(f32))
                spread = jnp.concatenate([jnp.where(part_of == k, folded, 0.0) for k in range(OWNERS)], axis=0)
                slot = sq_end.at[c, ra * OWNERS + part_of]
                slot[:, :tc] = jnp.sum(spread.T, axis=0, keepdims=True)
                me = ra * (PLANES * CORES) + cb
                for d in range(1, n * PLANES * CORES):
                    other = lax.rem(me + d, n * PLANES * CORES)
                    send("closing", c, slot, slot, (other // (PLANES * CORES), lax.rem(other, PLANES * CORES)))

    def stage_h(b, c):
        @pl.when(owns)
        def _():
            take("spread", c, act.at[0, pl.ds(0, q)])

        @pl.when(adds & jnp.logical_not(middle))
        def _():
            take("spread", c, act.at[0, pl.ds(0, OWNERS * q)])

        @pl.when(adds)
        def _():
            view = streams[b + 1].at[pl.ds(c * tc, tc)]
            send("rows", c, view, view, partner)

    def stage_z(b, c):
        receive_rows(c)
        slots = n * OWNERS

        @pl.when(owns)
        def _():
            take("closing", c, sq_end.at[0, pl.ds(0, slots - 1)])

        @pl.when(jnp.logical_not(owns))
        def _():
            take("closing", c, sq_end.at[0, pl.ds(0, slots)])

        total = sq_end[c, 0, :, :tc]
        for k in range(1, slots):
            total = total + sq_end[c, k, :, :tc]
        whole = pl.ds(c * tc, tc)
        out_ref[whole, :] = (end[whole, :].astype(f32) * column(total)[:, :1] * gains[2][...].astype(f32)).astype(bf16)

    stages = dict(zip(LETTERS, (stage_a, stage_u, stage_s, stage_b, stage_v, stage_c, stage_r, stage_d, stage_w, stage_e,
                                stage_f, stage_g, stage_h, stage_z)))
    x_loads[0].wait()
    for c, b, s in order(chunks):
        stages[s](b, c)
    most = pl.ds(0, 3 * r * chunks)
    for group, view in enumerate((part.at[:, :, most], sq_in, part.at[:, 0, most], act)):
        sent(group, view)

    @pl.when(owns)
    def _():
        sent(4, act.at[0])
        sent(5, z_in)
        sent(6, sq_end.at[:, pl.ds(0, n * PLANES * CORES - 1)])

    @pl.when(adds & jnp.logical_not(middle))
    def _():
        sent(4, act)


def fused_body(n, devices, tc, width, hidden_states, gain_first, gate_first, up_first, down_first, gain_second, gate_second,
               up_second, down_second, gain_last):
    tokens, local = hidden_states.shape
    units = gate_first.shape[1]
    chunks = tokens // tc
    bf16 = jnp.bfloat16
    share = tokens // n
    vmem = pl.BlockSpec(memory_space=pltpu.VMEM)
    hbm = pl.BlockSpec(memory_space=pl.ANY)
    return pl.pallas_call(
        functools.partial(kernel, n, chunks, tc, width),
        out_shape=pltpu.VMEM((tokens, local), bf16),
        in_specs=[hbm, vmem, hbm, hbm, hbm, vmem, hbm, hbm, hbm, vmem],
        out_specs=vmem,
        scratch_shapes=[pltpu.VMEM(w.shape, bf16) for w in (gate_first, up_first, down_first, gate_second, up_second, down_second)]
        + [
            pltpu.VMEM((tokens, local), bf16),
            pltpu.VMEM((tokens, local), bf16),
            pltpu.VMEM((tokens, local), bf16),
            pltpu.VMEM((2, tokens, local), bf16),
            pltpu.VMEM((2, 2, tokens, units), bf16),
            pltpu.VMEM((2, 2, 2, share, units), bf16),
            pltpu.VMEM((2, 2, share, units), bf16),
            pltpu.VMEM((2, tokens, units), bf16),
            pltpu.VMEM((2, chunks, 1, LANES), jnp.float32),
            pltpu.VMEM((2, chunks, n - 1, 1, LANES), jnp.float32),
            pltpu.VMEM((chunks, n * devices, 1, LANES), jnp.float32),
            pltpu.VMEM((2, tokens, local), bf16),
            pltpu.VMEM((2, tokens, local), bf16),
            pltpu.VMEM((2, tokens, local), bf16),
            pltpu.VMEM((2, PLANES - 1, tokens // OWNERS, local), bf16),
            pltpu.SemaphoreType.DMA((2,)),
            pltpu.SemaphoreType.DMA((2, 3)),
            pltpu.SemaphoreType.DMA((max(GROUP.values()) + 1,)),
            pltpu.SemaphoreType.DMA((chunks, len(ROLES))),
        ],
        compiler_params=pltpu.CompilerParams(collective_id=0, has_side_effects=True),
    )(
        hidden_states, gain_first, gate_first, up_first, down_first,
        gain_second, gate_second, up_second, down_second, gain_last,
    )


def solution(mesh):
    in_specs = (
        P(None, "ra"),
        P("ra"),
        P("ra", "cb"),
        P("ra", "cb"),
        P("cb", "ra"),
        P("ra"),
        P("ra", "cb"),
        P("ra", "cb"),
        P("cb", "ra"),
        P("ra"),
    )

    def run(hidden_states, *rest):
        tokens, width = hidden_states.shape
        tc = plan(mesh, tokens, width, rest[1].shape[1])
        form = body
        if tc is not None:
            form = functools.partial(fused_body, mesh.shape["ra"], mesh.shape["cb"], tc, width)
        return jax.shard_map(form, mesh=mesh, in_specs=in_specs, out_specs=P(None, "ra"), check_vma=False)(hidden_states, *rest)

    return run
```

```python
import functools

import jax
import jax.numpy as jnp
from jax import lax
from jax.experimental import pallas as pl
from jax.experimental.pallas import tpu as pltpu
from jax.sharding import PartitionSpec as P

norm_eps = 1e-06
residual_weight = 0.25
branch_weight = 0.5


def half_step(stream, gain, w_gate, w_up, w_down):
    width = stream.shape[1] * lax.axis_size("ra")
    values = stream.astype(jnp.float32)
    local_squares = jnp.sum(values * values, axis=1)
    normed = (values * gain.astype(jnp.float32)).astype(jnp.bfloat16)
    gate_part = jnp.dot(normed, w_gate, preferred_element_type=jnp.float32)
    upper_part = jnp.dot(normed, w_up, preferred_element_type=jnp.float32)
    count_ra = lax.axis_size("ra")
    spread_squares = jnp.broadcast_to(local_squares[:, None], (stream.shape[0], count_ra))
    gate, upper, squares = (
        lax.psum_scatter(gate_part, "ra", scatter_dimension=1, tiled=True),
        lax.psum_scatter(upper_part, "ra", scatter_dimension=1, tiled=True),
        lax.psum_scatter(spread_squares, "ra", scatter_dimension=1, tiled=True),
    )
    scale = lax.rsqrt(squares / width + norm_eps)
    hidden = (jax.nn.silu(gate * scale) * (upper * scale)).astype(jnp.bfloat16)
    branch = jnp.dot(
        lax.all_gather(hidden, "ra", axis=1, tiled=True), w_down, preferred_element_type=jnp.float32
    )
    block = lax.psum_scatter(branch, "cb", scatter_dimension=0, tiled=True)
    count = block.shape[0]
    offset = lax.axis_index("cb") * count
    own_rows = lax.dynamic_slice_in_dim(values, offset, count, 0)
    updated = (residual_weight * own_rows + branch_weight * block).astype(jnp.bfloat16)
    return lax.all_gather(updated, "cb", axis=0, tiled=True)


def body(
    hidden_states,
    gain_first,
    gate_first,
    up_first,
    down_first,
    gain_second,
    gate_second,
    up_second,
    down_second,
    gain_last,
):
    first = half_step(hidden_states, gain_first, gate_first, up_first, down_first)
    second = half_step(first, gain_second, gate_second, up_second, down_second)
    width = second.shape[1] * lax.axis_size("ra")
    values = second.astype(jnp.float32)
    squares = lax.psum(jnp.sum(values * values, axis=1), "ra")
    scale = lax.rsqrt(squares / width + norm_eps)[:, None]
    return (values * scale * gain_last.astype(jnp.float32)).astype(jnp.bfloat16)


MESH = pl.DeviceIdType.MESH
CORES = 2
LANES = 128
SUBLANES = 8
PLANES = 4
OWNERS = 2
SIZES = (64, 64, 32, 32, 32, 32, 64, 32, 32)
LETTERS = "AUSBVCRDWEFGHZ"
ROLES = ("gate", "up", "sum", "squares", "left", "right", "hidden", "pair", "mix", "spread", "rows", "closing")
GROUP = {"gate": 0, "up": 0, "sum": 0, "squares": 1, "left": 2, "right": 2, "hidden": 2, "pair": 3, "rows": 3, "mix": 4, "spread": 5, "closing": 6}
LONG, HOP = ("gate", "up"), ("left", "right")
SEQUENCE = (0, 1, 2, 28, 29, 56, 57, 58, 3, 4, 30, 84, 85, 31, 112, 32, 140, 141, 5, 6, 60, 168, 169, 59, 33, 7, 8, 88, 34, 87, 196, 197, 86, 36, 35, 61, 62, 143, 144, 142, 9, 170, 224, 113, 89, 37, 64, 10, 172, 63, 171, 198, 145, 200, 225, 199, 92, 90, 38, 91, 114, 11, 115, 65, 173, 148, 116, 147, 146, 201, 226, 227, 228, 174, 66, 39, 93, 176, 175, 12, 94, 117, 118, 67, 202, 203, 149, 204, 14, 229, 230, 40, 150, 15, 95, 177, 16, 119, 68, 120, 178, 42, 43, 151, 205, 206, 44, 232, 18, 231, 17, 96, 70, 71, 179, 121, 45, 122, 46, 72, 98, 99, 152, 100, 207, 233, 234, 19, 74, 73, 180, 20, 47, 48, 123, 154, 101, 102, 155, 156, 22, 208, 235, 21, 75, 76, 182, 183, 184, 124, 210, 158, 211, 103, 236, 50, 49, 157, 23, 77, 212, 126, 127, 24, 185, 186, 78, 104, 238, 105, 239, 159, 106, 214, 213, 51, 52, 128, 130, 129, 187, 25, 240, 79, 80, 242, 241, 160, 107, 162, 108, 161, 215, 188, 53, 131, 189, 190, 216, 132, 243, 244, 81, 109, 217, 218, 163, 134, 164, 133, 191, 192, 246, 245, 26, 219, 220, 54, 135, 136, 165, 110, 247, 55, 248, 193, 82, 83, 27, 221, 137, 249, 194, 166, 222, 195, 223, 138, 139, 111, 167, 250, 251)


def plan(mesh, tokens, width, units):
    n, devices = mesh.shape["ra"], mesh.shape["cb"]
    if n != 4 or devices != PLANES * CORES or width % (n * LANES) or units % (devices * LANES):
        return None
    return SIZES if sum(SIZES) == tokens else None


def ring_index(position):
    return position ^ (position >> 1)


def order(chunks):
    stages = [(c, b, s) for c in range(chunks) for b in range(2) for s in range(len(LETTERS)) if b or LETTERS[s] != "Z"]
    if len(SEQUENCE) == len(stages):
        return [(x // 28, x // 14 % 2, LETTERS[x % 14]) for x in SEQUENCE]
    return [(c, b, LETTERS[s]) for b, s, c in sorted((b, s, c) for c, b, s in stages)]


def kernel(n, sizes, width, x_hbm, g1, wg1, wu1, wd1, g2, wg2, wu2, wd2, g3, out_ref,
           wg_a, wu_a, wd_a, wg_b, wu_b, wd_b, g1_ref, g2_ref, g3_ref, x_ref, mid, end, act, part, long_in, short_in, hid, sq_own, sq_in, sq_end,
           down, pair_in, mixed, z_in, g_sem, x_sem, w_sem, send_sem, recv_sem):
    f32, bf16 = jnp.float32, jnp.bfloat16
    ra, cb = lax.axis_index("ra"), lax.axis_index("cb")
    pos, z, core = ring_index(ra), cb // CORES, cb % CORES
    local, units = x_ref.shape[-1], hid.shape[-1]
    chunks, tokens = len(sizes), sum(sizes)
    starts = [sum(sizes[:c]) for c in range(chunks)]
    cut = (units // LANES + 1) // 2 * LANES
    middle = (z == 1) | (z == 2)
    adds = core == 1
    owns = adds & middle
    streams = (x_ref, mid, end)
    gains = (g1_ref, g2_ref, g3_ref)
    weights = ((wg_a, wu_a, wd_a), (wg_b, wu_b, wd_b))

    loads = [[pltpu.make_async_copy(src, dst, w_sem.at[b, i]) for i, (src, dst) in enumerate(zip(srcs, weights[b]))]
             for b, srcs in enumerate(((wg1, wu1, wd1), (wg2, wu2, wd2)))]
    first, others_x = pl.ds(0, starts[1]), pl.ds(starts[1], tokens - starts[1])
    g_loads = [pltpu.make_async_copy(src, dst, g_sem.at[i]) for i, (src, dst) in enumerate(zip((g1, g2, g3), gains))]
    x_loads = [pltpu.make_async_copy(x_hbm.at[part_x], x_ref.at[part_x], x_sem.at[i]) for i, part_x in enumerate((first, others_x))]
    early = (x_loads[0], g_loads[0])
    for load in early:
        load.start()
    loads[0][0].start()
    pending = {(b, i): loads[b][i] for b in range(2) for i in range(3)}

    def ready(b, i):
        if (b, i) in pending:
            pending.pop((b, i)).wait()

    def at(position):
        return lax.rem(position + 2 * n, n)

    def ring(position):
        return (ring_index(at(position)), cb)

    steps = (ring(pos + 1), ring(pos - 1))
    signs = (1, -1)
    partner = (ra, z * CORES + (1 - core))
    others = [ring(pos + d) for d in range(1, n)]
    layers = [(ra, lax.rem(z + d, PLANES) * CORES + core) for d in range(1, PLANES)]

    def layer(plane):
        return (ra, plane * CORES + core)

    barrier = pltpu.get_barrier_semaphore()
    peers = others + layers + [partner]
    for peer in peers:
        pl.semaphore_signal(barrier, inc=1, device_id=peer, device_id_type=MESH)

    def send(role, c, src, dst, device):
        pltpu.make_async_remote_copy(src_ref=src, dst_ref=dst, send_sem=send_sem.at[GROUP[role]], recv_sem=recv_sem.at[c, ROLES.index(role)],
                                     device_id=device, device_id_type=MESH).start()

    def take(role, c, view):
        copy = pltpu.make_async_remote_copy(src_ref=view, dst_ref=view, send_sem=send_sem.at[0], recv_sem=recv_sem.at[c, ROLES.index(role)],
                                            device_id=partner, device_id_type=MESH)
        copy.wait_recv()

    def sent(group, view):
        copy = pltpu.make_async_remote_copy(src_ref=view, dst_ref=view, send_sem=send_sem.at[group], recv_sem=recv_sem.at[0, 0],
                                            device_id=partner, device_id_type=MESH)
        copy.wait_send()

    greeted = []

    def rows(c, offset, count):
        return pl.ds(pl.multiple_of(starts[c] + offset, SUBLANES), count)

    def tokens_of(c, share=1):
        return pl.ds(starts[c] // share, sizes[c] // share)

    def half_of(c, owner, half):
        r = sizes[c] // n
        if r % (2 * SUBLANES):
            return rows(c, owner * r, r), pl.ds(half * cut, units - cut if half else cut)
        return rows(c, owner * r + half * (r // 2), r // 2), pl.ds(0, units)

    def receive_rows(c):
        @pl.when(jnp.logical_not(adds))
        def _():
            take("rows", c, act.at[0, pl.ds(0, sizes[c])])

    def stage_a(b, c):
        whole = tokens_of(c)
        if b:
            receive_rows(c)
        elif c and len(x_loads) > 1:
            for load in (x_loads.pop(), *g_loads[1:]):
                load.wait()
        values = streams[b][whole, :].astype(f32)
        act[b, whole, :] = (values * gains[b][...].astype(f32)).astype(bf16)
        project(b, c, 0)

    def stage_u(b, c):
        project(b, c, 1)

    def project(b, c, half):
        whole = tokens_of(c)
        ready(b, half)
        part[b, half, whole, :] = jnp.dot(act[b, whole, :], weights[b][half][...], preferred_element_type=f32).astype(bf16)
        if not greeted:
            greeted.append(True)
            pl.semaphore_wait(barrier, len(peers))
        r = sizes[c] // n
        send(LONG[half], c, part.at[b, half, rows(c, at(pos + 2) * r, r)], long_in.at[b, half, 0, tokens_of(c, n)], steps[half])
        if half and len(greeted) == 1:
            greeted.append(True)
            for load in loads[0][2:] + loads[1]:
                load.start()

    def fold(values):
        squares = values * values
        folded = squares[:, :LANES]
        for k in range(1, local // LANES):
            folded = folded + squares[:, k * LANES:(k + 1) * LANES]
        return folded

    def column(squares):
        return jnp.broadcast_to(lax.rsqrt(squares / width + norm_eps), (LANES, squares.shape[1])).T

    def send_squares(b, c, values):
        sq_own[b, c, :, :sizes[c]] = jnp.sum(fold(values).T, axis=0, keepdims=True)
        for d in range(n - 1):
            send("squares", c, sq_own.at[b, c], sq_in.at[b, c, d], others[d])

    def scales(b, c):
        total = sq_own[b, c, :, :sizes[c]]
        take("squares", c, sq_in.at[b, c])
        for d in range(n - 1):
            total = total + sq_in[b, c, d, :, :sizes[c]]
        return column(total)

    def stage_s(b, c):
        r = sizes[c] // n
        for side in range(2):
            half = 1 - side
            send("sum", c, part.at[b, half, rows(c, at(pos + signs[side]) * r, r)], short_in.at[b, half, tokens_of(c, n)], steps[side])
        send_squares(b, c, streams[b][tokens_of(c), :].astype(f32))

    def pass_on(b, c, half):
        r = sizes[c] // n
        take(LONG[half], c, short_in.at[0, 0, pl.ds(0, r)])
        owner = rows(c, at(pos + signs[half]) * r, r)
        box = tokens_of(c, n)
        part[b, half, owner, :] = (part[b, half, owner, :].astype(f32) + long_in[b, half, 0, box, :].astype(f32)).astype(bf16)
        send("sum", c, part.at[b, half, owner], long_in.at[b, half, 1, box], steps[half])

    def stage_b(b, c):
        pass_on(b, c, 0)

    def stage_v(b, c):
        pass_on(b, c, 1)

    def stage_c(b, c):
        r = sizes[c] // n
        spread = scales(b, c).reshape(n, r, LANES)
        scale = spread[0]
        for k in range(1, n):
            scale = jnp.where(pos == k, spread[k], scale)
        scale = scale[:, :1]
        own, box = rows(c, pos * r, r), tokens_of(c, n)
        take("sum", c, hid.at[0, pl.ds(0, sizes[c])])
        sums = []
        for half in range(2):
            sums.append((part[b, half, own, :].astype(f32) + short_in[b, half, box, :].astype(f32)
                         + long_in[b, half, 1, box, :].astype(f32)) * scale)
        hid[b, own, :] = (jax.nn.silu(sums[0]) * sums[1]).astype(bf16)
        views = [hid.at[(b, *half_of(c, pos, half))] for half in range(2)]
        for side in range(2):
            send(HOP[side], c, views[side], views[side], steps[side])

    def stage_r(b, c):
        views = [hid.at[(b, *half_of(c, pos, half))] for half in range(2)]
        for side in range(2):
            send("hidden", c, views[1 - side], views[1 - side], steps[side])

    def hop(b, c, side):
        view = hid.at[(b, *half_of(c, at(pos - signs[side]), side))]
        take(HOP[side], c, view)
        send("hidden", c, view, view, steps[side])

    def stage_d(b, c):
        hop(b, c, 0)

    def stage_w(b, c):
        hop(b, c, 1)

    def stage_e(b, c):
        whole = tokens_of(c)
        ready(b, 2)
        take("hidden", c, hid.at[0, pl.ds(0, sizes[c] // 2)])
        down[b, whole, :] = jnp.dot(hid[b, whole, :], weights[b][2][...], preferred_element_type=f32).astype(bf16)

        @pl.when(jnp.logical_not(adds))
        def _():
            send("pair", c, down.at[b, whole], pair_in.at[b, whole], partner)

    def stage_f(b, c):
        whole = tokens_of(c)

        def mix(plane):
            q = sizes[c] // OWNERS
            send("mix", c, mixed.at[b, rows(c, (plane - 1) * q, q)],
                 z_in.at[b, lax.rem(z - plane + PLANES, PLANES) - 1, tokens_of(c, OWNERS)], layer(plane))

        first_owner = jnp.where(z < 2, 2, 1)

        @pl.when(adds)
        def _():
            take("pair", c, act.at[0, whole])
            mixed[b, whole, :] = (down[b, whole, :].astype(f32) + pair_in[b, whole, :].astype(f32)).astype(bf16)
            mix(first_owner)

        @pl.when(adds & jnp.logical_not(middle))
        def _():
            mix(PLANES - 1 - first_owner)

    def stage_g(b, c):
        @pl.when(owns)
        def _():
            part_of, q = z - 1, sizes[c] // OWNERS
            own = rows(c, part_of * q, q)
            total = mixed[b, own, :].astype(f32)
            take("mix", c, act.at[0, pl.ds(0, (PLANES - 1) * q)])
            for d in range(PLANES - 1):
                total = total + z_in[b, d, tokens_of(c, OWNERS), :].astype(f32)
            after = streams[b + 1]
            rounded = (residual_weight * streams[b][own, :].astype(f32) + branch_weight * total).astype(bf16)
            after[own, :] = rounded
            view = after.at[own]
            if b:
                folded = fold(rounded.astype(f32))
                spread = jnp.concatenate([jnp.where(part_of == k, folded, 0.0) for k in range(OWNERS)], axis=0)
                slot = sq_end.at[c, ra * OWNERS + part_of]
                slot[:, :sizes[c]] = jnp.sum(spread.T, axis=0, keepdims=True)
                me = ra * (PLANES * CORES) + cb
                for d in range(1, n * PLANES * CORES):
                    other = lax.rem(me + d, n * PLANES * CORES)
                    send("closing", c, slot, slot, (other // (PLANES * CORES), lax.rem(other, PLANES * CORES)))
            near = jnp.where(z == 1, 0, PLANES - 1)
            for plane in (PLANES - 1 - near, near, PLANES - 1 - z):
                send("spread", c, view, view, layer(plane))

    def stage_h(b, c):
        @pl.when(owns)
        def _():
            take("spread", c, act.at[0, pl.ds(0, sizes[c] // OWNERS)])

        @pl.when(adds & jnp.logical_not(middle))
        def _():
            take("spread", c, act.at[0, pl.ds(0, sizes[c])])

        @pl.when(adds)
        def _():
            view = streams[b + 1].at[tokens_of(c)]
            send("rows", c, view, view, partner)

    def stage_z(b, c):
        receive_rows(c)
        slots = n * OWNERS

        @pl.when(owns)
        def _():
            take("closing", c, sq_end.at[0, pl.ds(0, slots - 1)])

        @pl.when(jnp.logical_not(owns))
        def _():
            take("closing", c, sq_end.at[0, pl.ds(0, slots)])

        total = sq_end[c, 0, :, :sizes[c]]
        for k in range(1, slots):
            total = total + sq_end[c, k, :, :sizes[c]]
        whole = tokens_of(c)
        out_ref[whole, :] = (end[whole, :].astype(f32) * column(total)[:, :1] * gains[2][...].astype(f32)).astype(bf16)

    stages = dict(zip(LETTERS, (stage_a, stage_u, stage_s, stage_b, stage_v, stage_c, stage_r, stage_d, stage_w, stage_e,
                                stage_f, stage_g, stage_h, stage_z)))
    for load in early:
        load.wait()
    for load in (loads[0][1], x_loads[1], *g_loads[1:]):
        load.start()
    for c, b, s in order(chunks):
        stages[s](b, c)
    most = pl.ds(0, 3 * tokens // n)
    for group, view in enumerate((part.at[:, :, most], sq_in, part.at[:, 0, most], act)):
        sent(group, view)

    @pl.when(owns)
    def _():
        sent(4, act.at[0])
        sent(5, z_in)
        sent(6, sq_end.at[:, pl.ds(0, n * PLANES * CORES - 1)])

    @pl.when(adds & jnp.logical_not(middle))
    def _():
        sent(4, act)


def fused_body(n, devices, sizes, width, hidden_states, gain_first, gate_first, up_first, down_first, gain_second, gate_second,
               up_second, down_second, gain_last):
    tokens, local = hidden_states.shape
    units = gate_first.shape[1]
    chunks = len(sizes)
    bf16 = jnp.bfloat16
    share = tokens // n
    vmem = pl.BlockSpec(memory_space=pltpu.VMEM)
    hbm = pl.BlockSpec(memory_space=pl.ANY)
    return pl.pallas_call(
        functools.partial(kernel, n, sizes, width),
        out_shape=pltpu.VMEM((tokens, local), bf16),
        in_specs=[hbm] * 10,
        out_specs=vmem,
        scratch_shapes=[pltpu.VMEM(w.shape, bf16) for w in (gate_first, up_first, down_first, gate_second, up_second, down_second)]
        + [pltpu.VMEM((local,), bf16)] * 3
        + [
            pltpu.VMEM((tokens, local), bf16),
            pltpu.VMEM((tokens, local), bf16),
            pltpu.VMEM((tokens, local), bf16),
            pltpu.VMEM((2, tokens, local), bf16),
            pltpu.VMEM((2, 2, tokens, units), bf16),
            pltpu.VMEM((2, 2, 2, share, units), bf16),
            pltpu.VMEM((2, 2, share, units), bf16),
            pltpu.VMEM((2, tokens, units), bf16),
            pltpu.VMEM((2, chunks, 1, LANES), jnp.float32),
            pltpu.VMEM((2, chunks, n - 1, 1, LANES), jnp.float32),
            pltpu.VMEM((chunks, n * devices, 1, LANES), jnp.float32),
            pltpu.VMEM((2, tokens, local), bf16),
            pltpu.VMEM((2, tokens, local), bf16),
            pltpu.VMEM((2, tokens, local), bf16),
            pltpu.VMEM((2, PLANES - 1, tokens // OWNERS, local), bf16),
            pltpu.SemaphoreType.DMA((3,)),
            pltpu.SemaphoreType.DMA((2,)),
            pltpu.SemaphoreType.DMA((2, 3)),
            pltpu.SemaphoreType.DMA((max(GROUP.values()) + 1,)),
            pltpu.SemaphoreType.DMA((chunks, len(ROLES))),
        ],
        compiler_params=pltpu.CompilerParams(collective_id=0, has_side_effects=True),
    )(
        hidden_states, gain_first, gate_first, up_first, down_first,
        gain_second, gate_second, up_second, down_second, gain_last,
    )


def solution(mesh):
    in_specs = (
        P(None, "ra"),
        P("ra"),
        P("ra", "cb"),
        P("ra", "cb"),
        P("cb", "ra"),
        P("ra"),
        P("ra", "cb"),
        P("ra", "cb"),
        P("cb", "ra"),
        P("ra"),
    )

    def run(hidden_states, *rest):
        tokens, width = hidden_states.shape
        sizes = plan(mesh, tokens, width, rest[1].shape[1])
        form = body
        if sizes is not None:
            form = functools.partial(fused_body, mesh.shape["ra"], mesh.shape["cb"], sizes, width)
        return jax.shard_map(form, mesh=mesh, in_specs=in_specs, out_specs=P(None, "ra"), check_vma=False)(hidden_states, *rest)

    return run
```

```python
import functools

import jax
import jax.numpy as jnp
from jax import lax
from jax.experimental import pallas as pl
from jax.experimental.pallas import tpu as pltpu
from jax.sharding import PartitionSpec as P

norm_eps = 1e-06
residual_weight = 0.25
branch_weight = 0.5


def half_step(stream, gain, w_gate, w_up, w_down):
    width = stream.shape[1] * lax.axis_size("ra")
    values = stream.astype(jnp.float32)
    local_squares = jnp.sum(values * values, axis=1)
    normed = (values * gain.astype(jnp.float32)).astype(jnp.bfloat16)
    gate_part = jnp.dot(normed, w_gate, preferred_element_type=jnp.float32)
    upper_part = jnp.dot(normed, w_up, preferred_element_type=jnp.float32)
    count_ra = lax.axis_size("ra")
    spread_squares = jnp.broadcast_to(local_squares[:, None], (stream.shape[0], count_ra))
    gate, upper, squares = (
        lax.psum_scatter(gate_part, "ra", scatter_dimension=1, tiled=True),
        lax.psum_scatter(upper_part, "ra", scatter_dimension=1, tiled=True),
        lax.psum_scatter(spread_squares, "ra", scatter_dimension=1, tiled=True),
    )
    scale = lax.rsqrt(squares / width + norm_eps)
    hidden = (jax.nn.silu(gate * scale) * (upper * scale)).astype(jnp.bfloat16)
    branch = jnp.dot(
        lax.all_gather(hidden, "ra", axis=1, tiled=True), w_down, preferred_element_type=jnp.float32
    )
    block = lax.psum_scatter(branch, "cb", scatter_dimension=0, tiled=True)
    count = block.shape[0]
    offset = lax.axis_index("cb") * count
    own_rows = lax.dynamic_slice_in_dim(values, offset, count, 0)
    updated = (residual_weight * own_rows + branch_weight * block).astype(jnp.bfloat16)
    return lax.all_gather(updated, "cb", axis=0, tiled=True)


def body(
    hidden_states,
    gain_first,
    gate_first,
    up_first,
    down_first,
    gain_second,
    gate_second,
    up_second,
    down_second,
    gain_last,
):
    first = half_step(hidden_states, gain_first, gate_first, up_first, down_first)
    second = half_step(first, gain_second, gate_second, up_second, down_second)
    width = second.shape[1] * lax.axis_size("ra")
    values = second.astype(jnp.float32)
    squares = lax.psum(jnp.sum(values * values, axis=1), "ra")
    scale = lax.rsqrt(squares / width + norm_eps)[:, None]
    return (values * scale * gain_last.astype(jnp.float32)).astype(jnp.bfloat16)


MESH = pl.DeviceIdType.MESH
CORES = 2
LANES = 128
SUBLANES = 8
PLANES = 4
OWNERS = 2
SIZES = (64, 64, 32, 32, 32, 32, 64, 32, 32)
LETTERS = "AUSBVCRDWEFGHZ"
ROLES = ("gate", "up", "sum", "squares", "left", "right", "hidden", "pair", "mix", "spread", "rows", "closing")
GROUP = {"gate": 0, "up": 0, "sum": 0, "squares": 1, "left": 2, "right": 2, "hidden": 2, "pair": 3, "rows": 3, "mix": 4, "spread": 5, "closing": 6}
LONG, HOP = ("gate", "up"), ("left", "right")
SEQUENCE = (0, 1, 2, 28, 29, 56, 57, 58, 3, 4, 30, 84, 85, 31, 112, 32, 140, 141, 5, 6, 60, 168, 169, 59, 33, 7, 8, 88, 34, 87, 196, 197, 86, 36, 35, 61, 62, 143, 144, 142, 9, 170, 224, 113, 89, 37, 64, 10, 172, 63, 171, 198, 145, 200, 225, 199, 92, 90, 38, 91, 114, 11, 115, 65, 173, 148, 116, 147, 146, 201, 226, 227, 228, 174, 66, 39, 93, 176, 175, 12, 94, 117, 118, 67, 202, 203, 149, 204, 14, 229, 230, 40, 150, 15, 95, 177, 16, 119, 68, 120, 178, 42, 43, 151, 205, 206, 44, 232, 18, 231, 17, 96, 70, 71, 179, 121, 45, 122, 46, 72, 98, 99, 152, 100, 207, 233, 234, 19, 74, 73, 180, 20, 47, 48, 123, 154, 101, 102, 155, 156, 22, 208, 235, 21, 75, 76, 182, 183, 184, 124, 210, 158, 211, 103, 236, 50, 49, 157, 23, 77, 212, 126, 127, 24, 185, 186, 78, 104, 238, 105, 239, 159, 106, 214, 213, 51, 52, 128, 130, 129, 187, 25, 240, 79, 80, 242, 241, 160, 107, 162, 108, 161, 215, 188, 53, 131, 189, 190, 216, 132, 243, 244, 81, 109, 217, 218, 163, 134, 164, 133, 191, 192, 246, 245, 26, 219, 220, 54, 135, 136, 165, 110, 247, 55, 248, 193, 82, 83, 27, 221, 137, 249, 194, 166, 222, 195, 223, 138, 139, 111, 167, 250, 251)


def plan(mesh, tokens, width, units):
    n, devices = mesh.shape["ra"], mesh.shape["cb"]
    if n != 4 or devices != PLANES * CORES or width % (n * LANES) or units % (devices * LANES):
        return None
    return SIZES if sum(SIZES) == tokens else None


def ring_index(position):
    return position ^ (position >> 1)


def order(chunks):
    stages = [(c, b, s) for c in range(chunks) for b in range(2) for s in range(len(LETTERS)) if b or LETTERS[s] != "Z"]
    if len(SEQUENCE) == len(stages):
        return [(x // 28, x // 14 % 2, LETTERS[x % 14]) for x in SEQUENCE]
    return [(c, b, LETTERS[s]) for b, s, c in sorted((b, s, c) for c, b, s in stages)]


def kernel(n, sizes, width, x_hbm, g1, wg1, wu1, wd1, g2, wg2, wu2, wd2, g3, out_ref,
           wg_a, wu_a, wd_a, wg_b, wu_b, wd_b, g1_ref, g2_ref, g3_ref, x_ref, mid, end, act, part, long_in, short_in, hid, sq_own, sq_in, sq_end, sq_all,
           down, pair_in, mixed, z_in, g_sem, x_sem, w_sem, send_sem, recv_sem):
    f32, bf16 = jnp.float32, jnp.bfloat16
    ra, cb = lax.axis_index("ra"), lax.axis_index("cb")
    pos, z, core = ring_index(ra), cb // CORES, cb % CORES
    local, units = x_ref.shape[-1], hid.shape[-1]
    chunks, tokens = len(sizes), sum(sizes)
    starts = [sum(sizes[:c]) for c in range(chunks)]
    cut = (units // LANES + 1) // 2 * LANES
    middle = (z == 1) | (z == 2)
    adds = core == 1
    owns = adds & middle
    streams = (x_ref, mid, end)
    gains = (g1_ref, g2_ref, g3_ref)
    weights = ((wg_a, wu_a, wd_a), (wg_b, wu_b, wd_b))

    loads = [[pltpu.make_async_copy(src, dst, w_sem.at[b, i]) for i, (src, dst) in enumerate(zip(srcs, weights[b]))]
             for b, srcs in enumerate(((wg1, wu1, wd1), (wg2, wu2, wd2)))]
    first, others_x = pl.ds(0, starts[1]), pl.ds(starts[1], tokens - starts[1])
    g_loads = [pltpu.make_async_copy(src, dst, g_sem.at[i]) for i, (src, dst) in enumerate(zip((g1, g2, g3), gains))]
    x_loads = [pltpu.make_async_copy(x_hbm.at[part_x], x_ref.at[part_x], x_sem.at[i]) for i, part_x in enumerate((first, others_x))]
    early = (x_loads[0], g_loads[0])
    for load in early:
        load.start()
    loads[0][0].start()
    pending = {(b, i): loads[b][i] for b in range(2) for i in range(3)}

    def ready(b, i):
        if (b, i) in pending:
            pending.pop((b, i)).wait()

    def at(position):
        return lax.rem(position + 2 * n, n)

    def ring(position):
        return (ring_index(at(position)), cb)

    steps = (ring(pos + 1), ring(pos - 1))
    signs = (1, -1)
    partner = (ra, z * CORES + (1 - core))
    others = [ring(pos + d) for d in range(1, n)]
    layers = [(ra, lax.rem(z + d, PLANES) * CORES + core) for d in range(1, PLANES)]

    def layer(plane):
        return (ra, plane * CORES + core)

    barrier = pltpu.get_barrier_semaphore()
    peers = others + layers + [partner]
    for peer in peers:
        pl.semaphore_signal(barrier, inc=1, device_id=peer, device_id_type=MESH)

    def send(role, c, src, dst, device):
        pltpu.make_async_remote_copy(src_ref=src, dst_ref=dst, send_sem=send_sem.at[GROUP[role]], recv_sem=recv_sem.at[c, ROLES.index(role)],
                                     device_id=device, device_id_type=MESH).start()

    def take(role, c, view):
        copy = pltpu.make_async_remote_copy(src_ref=view, dst_ref=view, send_sem=send_sem.at[0], recv_sem=recv_sem.at[c, ROLES.index(role)],
                                            device_id=partner, device_id_type=MESH)
        copy.wait_recv()

    def sent(group, view):
        copy = pltpu.make_async_remote_copy(src_ref=view, dst_ref=view, send_sem=send_sem.at[group], recv_sem=recv_sem.at[0, 0],
                                            device_id=partner, device_id_type=MESH)
        copy.wait_send()

    greeted = []

    def rows(c, offset, count):
        return pl.ds(pl.multiple_of(starts[c] + offset, SUBLANES), count)

    def tokens_of(c, share=1):
        return pl.ds(starts[c] // share, sizes[c] // share)

    def half_of(c, owner, half):
        r = sizes[c] // n
        if r % (2 * SUBLANES):
            return rows(c, owner * r, r), pl.ds(half * cut, units - cut if half else cut)
        return rows(c, owner * r + half * (r // 2), r // 2), pl.ds(0, units)

    def receive_rows(c):
        @pl.when(jnp.logical_not(adds))
        def _():
            take("rows", c, act.at[0, pl.ds(0, sizes[c])])

    def stage_a(b, c):
        whole = tokens_of(c)
        if b:
            receive_rows(c)
        elif c and len(x_loads) > 1:
            for load in (x_loads.pop(), *g_loads[1:]):
                load.wait()
        values = streams[b][whole, :].astype(f32)
        act[b, whole, :] = (values * gains[b][...].astype(f32)).astype(bf16)
        project(b, c, 0)

    def stage_u(b, c):
        project(b, c, 1)

    def project(b, c, half):
        whole = tokens_of(c)
        ready(b, half)
        part[b, half, whole, :] = jnp.dot(act[b, whole, :], weights[b][half][...], preferred_element_type=f32).astype(bf16)
        if not greeted:
            greeted.append(True)
            pl.semaphore_wait(barrier, len(peers))
        r = sizes[c] // n
        send(LONG[half], c, part.at[b, half, rows(c, at(pos + 2) * r, r)], long_in.at[b, half, 0, tokens_of(c, n)], steps[half])
        if half and len(greeted) == 1:
            greeted.append(True)
            for load in loads[0][2:] + loads[1]:
                load.start()

    def fold(values):
        squares = values * values
        folded = squares[:, :LANES]
        for k in range(1, local // LANES):
            folded = folded + squares[:, k * LANES:(k + 1) * LANES]
        return folded

    def column(squares):
        return jnp.broadcast_to(lax.rsqrt(squares / width + norm_eps), (LANES, squares.shape[1])).T

    def send_squares(b, c, values):
        sq_own[b, c, :, :sizes[c]] = jnp.sum(fold(values).T, axis=0, keepdims=True)
        for d in range(n - 1):
            send("squares", c, sq_own.at[b, c], sq_in.at[b, c, d], others[d])

    def scales(b, c):
        total = sq_own[b, c, :, :sizes[c]]
        take("squares", c, sq_in.at[b, c])
        for d in range(n - 1):
            total = total + sq_in[b, c, d, :, :sizes[c]]
        return column(total)

    def stage_s(b, c):
        r = sizes[c] // n
        for side in range(2):
            half = 1 - side
            send("sum", c, part.at[b, half, rows(c, at(pos + signs[side]) * r, r)], short_in.at[b, half, tokens_of(c, n)], steps[side])
        send_squares(b, c, streams[b][tokens_of(c), :].astype(f32))

    def pass_on(b, c, half):
        r = sizes[c] // n
        take(LONG[half], c, short_in.at[0, 0, pl.ds(0, r)])
        owner = rows(c, at(pos + signs[half]) * r, r)
        box = tokens_of(c, n)
        part[b, half, owner, :] = (part[b, half, owner, :].astype(f32) + long_in[b, half, 0, box, :].astype(f32)).astype(bf16)
        send("sum", c, part.at[b, half, owner], long_in.at[b, half, 1, box], steps[half])

    def stage_b(b, c):
        pass_on(b, c, 0)

    def stage_v(b, c):
        pass_on(b, c, 1)

    def stage_c(b, c):
        r = sizes[c] // n
        spread = scales(b, c).reshape(n, r, LANES)
        scale = spread[0]
        for k in range(1, n):
            scale = jnp.where(pos == k, spread[k], scale)
        scale = scale[:, :1]
        own, box = rows(c, pos * r, r), tokens_of(c, n)
        take("sum", c, hid.at[0, pl.ds(0, sizes[c])])
        sums = []
        for half in range(2):
            sums.append((part[b, half, own, :].astype(f32) + short_in[b, half, box, :].astype(f32)
                         + long_in[b, half, 1, box, :].astype(f32)) * scale)
        hid[b, own, :] = (jax.nn.silu(sums[0]) * sums[1]).astype(bf16)
        views = [hid.at[(b, *half_of(c, pos, half))] for half in range(2)]
        for side in range(2):
            send(HOP[side], c, views[side], views[side], steps[side])

    def stage_r(b, c):
        views = [hid.at[(b, *half_of(c, pos, half))] for half in range(2)]
        for side in range(2):
            send("hidden", c, views[1 - side], views[1 - side], steps[side])

    def hop(b, c, side):
        view = hid.at[(b, *half_of(c, at(pos - signs[side]), side))]
        take(HOP[side], c, view)
        send("hidden", c, view, view, steps[side])

    def stage_d(b, c):
        hop(b, c, 0)

    def stage_w(b, c):
        hop(b, c, 1)

    def stage_e(b, c):
        whole = tokens_of(c)
        ready(b, 2)
        take("hidden", c, hid.at[0, pl.ds(0, sizes[c] // 2)])
        down[b, whole, :] = jnp.dot(hid[b, whole, :], weights[b][2][...], preferred_element_type=f32).astype(bf16)

        @pl.when(jnp.logical_not(adds))
        def _():
            send("pair", c, down.at[b, whole], pair_in.at[b, whole], partner)

    def stage_f(b, c):
        whole = tokens_of(c)

        def mix(plane):
            q = sizes[c] // OWNERS
            send("mix", c, mixed.at[b, rows(c, (plane - 1) * q, q)],
                 z_in.at[b, lax.rem(z - plane + PLANES, PLANES) - 1, tokens_of(c, OWNERS)], layer(plane))

        first_owner = jnp.where(z < 2, 2, 1)

        @pl.when(adds)
        def _():
            take("pair", c, act.at[0, whole])
            mixed[b, whole, :] = (down[b, whole, :].astype(f32) + pair_in[b, whole, :].astype(f32)).astype(bf16)
            mix(first_owner)

        @pl.when(adds & jnp.logical_not(middle))
        def _():
            mix(PLANES - 1 - first_owner)

    def stage_g(b, c):
        @pl.when(owns)
        def _():
            part_of, q = z - 1, sizes[c] // OWNERS
            own = rows(c, part_of * q, q)
            total = mixed[b, own, :].astype(f32)
            take("mix", c, act.at[0, pl.ds(0, (PLANES - 1) * q)])
            for d in range(PLANES - 1):
                total = total + z_in[b, d, tokens_of(c, OWNERS), :].astype(f32)
            after = streams[b + 1]
            rounded = (residual_weight * streams[b][own, :].astype(f32) + branch_weight * total).astype(bf16)
            after[own, :] = rounded
            view = after.at[own]
            if b:
                folded = fold(rounded.astype(f32))
                spread = jnp.concatenate([jnp.where(part_of == k, folded, 0.0) for k in range(OWNERS)], axis=0)
                slot = sq_end.at[c, ra * OWNERS + part_of]
                slot[:, :sizes[c]] = jnp.sum(spread.T, axis=0, keepdims=True)
                me = ra * PLANES + z
                for d in range(1, n * PLANES):
                    other = lax.rem(me + d, n * PLANES)
                    send("closing", c, slot, slot, (other // PLANES, lax.rem(other, PLANES) * CORES + core))
            near = jnp.where(z == 1, 0, PLANES - 1)
            for plane in (PLANES - 1 - near, near, PLANES - 1 - z):
                send("spread", c, view, view, layer(plane))

    def stage_h(b, c):
        @pl.when(owns)
        def _():
            take("spread", c, act.at[0, pl.ds(0, sizes[c] // OWNERS)])

        @pl.when(adds & jnp.logical_not(middle))
        def _():
            take("spread", c, act.at[0, pl.ds(0, sizes[c])])

        @pl.when(adds)
        def _():
            view = streams[b + 1].at[tokens_of(c)]
            send("rows", c, view, view, partner)

        slots = n * OWNERS
        if b:
            @pl.when(owns)
            def _():
                take("closing", c, sq_end.at[0, pl.ds(0, slots - 1)])

            @pl.when(adds & jnp.logical_not(middle))
            def _():
                take("closing", c, sq_end.at[0, pl.ds(0, slots)])

            @pl.when(adds)
            def _():
                total = sq_end[c, 0]
                for k in range(1, slots):
                    total = total + sq_end[c, k]
                sq_all[c] = total
                send("closing", c, sq_all.at[c], sq_all.at[c], partner)

    def stage_z(b, c):
        receive_rows(c)

        @pl.when(jnp.logical_not(adds))
        def _():
            take("closing", c, sq_all.at[0])

        whole = tokens_of(c)
        out_ref[whole, :] = (end[whole, :].astype(f32) * column(sq_all[c, :, :sizes[c]])[:, :1] * gains[2][...].astype(f32)).astype(bf16)

    stages = dict(zip(LETTERS, (stage_a, stage_u, stage_s, stage_b, stage_v, stage_c, stage_r, stage_d, stage_w, stage_e,
                                stage_f, stage_g, stage_h, stage_z)))
    for load in early:
        load.wait()
    for load in (loads[0][1], x_loads[1], *g_loads[1:]):
        load.start()
    for c, b, s in order(chunks):
        stages[s](b, c)
    most = pl.ds(0, 3 * tokens // n)
    for group, view in enumerate((part.at[:, :, most], sq_in, part.at[:, 0, most], act)):
        sent(group, view)

    @pl.when(owns)
    def _():
        sent(4, act.at[0])
        sent(5, z_in)
        sent(6, sq_end)

    @pl.when(adds & jnp.logical_not(middle))
    def _():
        sent(4, act)
        sent(6, sq_all)


def fused_body(n, devices, sizes, width, hidden_states, gain_first, gate_first, up_first, down_first, gain_second, gate_second,
               up_second, down_second, gain_last):
    tokens, local = hidden_states.shape
    units = gate_first.shape[1]
    chunks = len(sizes)
    bf16 = jnp.bfloat16
    share = tokens // n
    vmem = pl.BlockSpec(memory_space=pltpu.VMEM)
    hbm = pl.BlockSpec(memory_space=pl.ANY)
    return pl.pallas_call(
        functools.partial(kernel, n, sizes, width),
        out_shape=pltpu.VMEM((tokens, local), bf16),
        in_specs=[hbm] * 10,
        out_specs=vmem,
        scratch_shapes=[pltpu.VMEM(w.shape, bf16) for w in (gate_first, up_first, down_first, gate_second, up_second, down_second)]
        + [pltpu.VMEM((local,), bf16)] * 3
        + [
            pltpu.VMEM((tokens, local), bf16),
            pltpu.VMEM((tokens, local), bf16),
            pltpu.VMEM((tokens, local), bf16),
            pltpu.VMEM((2, tokens, local), bf16),
            pltpu.VMEM((2, 2, tokens, units), bf16),
            pltpu.VMEM((2, 2, 2, share, units), bf16),
            pltpu.VMEM((2, 2, share, units), bf16),
            pltpu.VMEM((2, tokens, units), bf16),
            pltpu.VMEM((2, chunks, 1, LANES), jnp.float32),
            pltpu.VMEM((2, chunks, n - 1, 1, LANES), jnp.float32),
            pltpu.VMEM((chunks, n * PLANES, 1, LANES), jnp.float32),
            pltpu.VMEM((chunks, 1, LANES), jnp.float32),
            pltpu.VMEM((2, tokens, local), bf16),
            pltpu.VMEM((2, tokens, local), bf16),
            pltpu.VMEM((2, tokens, local), bf16),
            pltpu.VMEM((2, PLANES - 1, tokens // OWNERS, local), bf16),
            pltpu.SemaphoreType.DMA((3,)),
            pltpu.SemaphoreType.DMA((2,)),
            pltpu.SemaphoreType.DMA((2, 3)),
            pltpu.SemaphoreType.DMA((max(GROUP.values()) + 1,)),
            pltpu.SemaphoreType.DMA((chunks, len(ROLES))),
        ],
        compiler_params=pltpu.CompilerParams(collective_id=0, has_side_effects=True),
    )(
        hidden_states, gain_first, gate_first, up_first, down_first,
        gain_second, gate_second, up_second, down_second, gain_last,
    )


def solution(mesh):
    in_specs = (
        P(None, "ra"),
        P("ra"),
        P("ra", "cb"),
        P("ra", "cb"),
        P("cb", "ra"),
        P("ra"),
        P("ra", "cb"),
        P("ra", "cb"),
        P("cb", "ra"),
        P("ra"),
    )

    def run(hidden_states, *rest):
        tokens, width = hidden_states.shape
        sizes = plan(mesh, tokens, width, rest[1].shape[1])
        form = body
        if sizes is not None:
            form = functools.partial(fused_body, mesh.shape["ra"], mesh.shape["cb"], sizes, width)
        return jax.shard_map(form, mesh=mesh, in_specs=in_specs, out_specs=P(None, "ra"), check_vma=False)(hidden_states, *rest)

    return run
```
